32 devices in a mesh: sp: 8 (over z, y), tp: 4 (over x, core).
Axes of the slice: x: 2, y: 2, z: 4, core: 2. Of those that a mesh axis runs over, the one named last changes fastest.
Arguments:
- tokens: bfloat16 [4096, 2048], P(('sp', 'tp')), may hold values from -6 to 6
- norm_gain: float32 [2048], replicated, may hold values from 0.25 to 5
- w_query_one: bfloat16 [2048, 512], P(None, 'tp'), may hold values from -0.21875 to 0.21875
- w_query_two: bfloat16 [2048, 512], P(None, 'tp'), may hold values from -0.21875 to 0.21875
- w_key_one: bfloat16 [2048, 512], P(None, 'tp'), may hold values from -0.125 to 0.125
- w_key_two: bfloat16 [2048, 512], P(None, 'tp'), may hold values from -0.125 to 0.125
- w_value: bfloat16 [2048, 1024], P(None, 'tp'), may hold values from -0.125 to 0.125
- mix_lambda: float32 [8], P('tp'), may hold values from 0.3 to 0.8
- head_gain: float32 [128], replicated, may hold values from 0.1 to 1.9
- w_ret_query: bfloat16 [2048, 512], P(None, 'tp'), may hold values from -0.125 to 0.125
- w_ret_key: bfloat16 [2048, 512], P(None, 'tp'), may hold values from -0.125 to 0.125
- w_ret_value: bfloat16 [2048, 1024], P(None, 'tp'), may hold values from -0.125 to 0.125
- retain_log: float32 [8, 4096], P('tp', 'sp'), may hold values from -1 to 0
- init_state: float32 [8, 64, 128], P('tp'), may hold values from -144 to 144
- w_out_diff: bfloat16 [1024, 2048], P('tp'), may hold values from -0.125 to 0.125
- w_out_ret: bfloat16 [1024, 2048], P('tp'), may hold values from -0.125 to 0.125
Outputs:
- mixed: bfloat16 [4096, 2048], P(('sp', 'tp'))
The draws below stay inside these ranges and needn't reach their ends.
All inputs are finite; a program needn't handle non-finite values.
Results may differ from the reference program's by a relative error of at most 0.015.
The reference program's roundings to bfloat16 on the way count: a program that leaves them out, or rounds other values in their place, can miss the bound.
Values may be sent and summed in bfloat16 or wider, within the bound.
No kernel may reach another device: no remote copies, remote signals or barrier semaphores. Data moves between devices by JAX's collectives and lax.ppermute only.
A program may use at most 128 MiB of HBM per device.

```python
import math
import jax
import jax.numpy as jnp
from jax import lax

D = 2048
HEADS_DIFF = 8
HEADS_RET = 8
HEAD = 64
VAL = 128
BLOCK = 256
TOK_DEV = 512
TOKENS = 4096


def draw_retain_log(key, part):
    keys = jax.random.split(jax.random.fold_in(key, 11), 7)
    slow = jax.random.bernoulli(keys[0], 0.5, (HEADS_RET,))
    slow_rate = jax.random.uniform(keys[1], (HEADS_RET,), minval=0.1, maxval=0.3) / TOKENS
    fast_rate = jnp.exp(jax.random.uniform(keys[2], (HEADS_RET,), minval=math.log(1.0 / 100.0), maxval=math.log(1.0 / 30.0)))
    fading_speed = jnp.where(slow, slow_rate, fast_rate)
    pace = jnp.exp(jax.random.uniform(keys[3], (TOKENS // TOK_DEV,), minval=-0.7, maxval=0.7))
    fading_speeds_list = jnp.repeat(pace, TOK_DEV)
    sampled_displacement = jnp.exp(jax.random.uniform(keys[4], (HEADS_RET, TOKENS), minval=-0.5, maxval=0.5))
    sequence_indices = jax.random.randint(keys[5], (HEADS_RET, 3), 0, TOKENS)
    stack_level = jnp.log(jax.random.uniform(keys[6], (HEADS_RET, 3), minval=0.5, maxval=0.8))
    sequence_index = jnp.arange(TOKENS, dtype=jnp.int32)
    cluster_sets = jnp.sum(jnp.where(sequence_index[None, None, :] == sequence_indices[:, :, None], stack_level[:, :, None], 0.0), axis=1)
    return (-fading_speed[:, None] * fading_speeds_list[None, :] * sampled_displacement + cluster_sets).astype(jnp.float32)


def draw_norm_gain(key, part):
    inner = jax.random.fold_in(key, 23)
    gains = 1.0 + 0.18 * jax.random.truncated_normal(inner, -4.0, 4.0, (D,))
    return gains.astype(jnp.float32)


def block_levels(stream_key, extent, pieces, low, largest):
    loudness, own = 1.0, jax.random.fold_in(stream_key, 6)
    for axis_at, parts in pieces:
        steps = jnp.exp(jax.random.uniform(jax.random.fold_in(own, axis_at), (parts,), jnp.float32, low / len(pieces), largest / len(pieces)))
        loudness = loudness * jnp.repeat(steps, extent[axis_at] // parts).reshape([-1 if axis == axis_at else 1 for axis in range(len(extent))])
    return loudness


def normal_values(own_key, dims, width, most, cuts=(), kind=jnp.bfloat16):
    gain = block_levels(own_key, dims, cuts, -0.22, 0.18) if cuts else 1.0
    entries = jax.random.normal(own_key, dims, jnp.float32) * width * gain
    return jnp.minimum(jnp.maximum(entries, -most), most).astype(kind)


def setup_inputs(seed: int = 0) -> dict:
    seeds = jax.random.split(jax.random.key(seed), 17)
    return {
        "tokens": normal_values(seeds[0], (TOKENS, D), 1.0, 6.0, ((0, 32),)),
        "norm_gain": draw_norm_gain(jax.random.fold_in(seeds[16], 71), 0),
        "w_query_one": normal_values(seeds[2], (D, HEADS_DIFF * HEAD), (D // 3) ** -0.5, 0.21875, ((1, 4),)),
        "w_query_two": normal_values(seeds[3], (D, HEADS_DIFF * HEAD), (D // 3) ** -0.5, 0.21875, ((1, 4),)),
        "w_key_one": normal_values(seeds[4], (D, HEADS_DIFF * HEAD), D ** -0.5, 0.125, ((1, 4),)),
        "w_key_two": normal_values(seeds[5], (D, HEADS_DIFF * HEAD), D ** -0.5, 0.125, ((1, 4),)),
        "w_value": normal_values(seeds[6], (D, HEADS_DIFF * VAL), D ** -0.5, 0.125, ((1, 4),)),
        "mix_lambda": jnp.clip(0.3 + 0.5 * jax.random.uniform(seeds[7], (HEADS_DIFF,), jnp.float32) ** block_levels(seeds[7], (HEADS_DIFF,), ((0, 4),), -0.2, 0.2), 0.3, 0.8),
        "head_gain": jnp.clip(1.0 + 0.18 * jax.random.normal(seeds[8], (VAL,), jnp.float32), 0.1, 1.9),
        "w_ret_query": normal_values(seeds[9], (D, HEADS_RET * HEAD), D ** -0.5, 0.125, ((1, 4),)),
        "w_ret_key": normal_values(seeds[10], (D, HEADS_RET * HEAD), D ** -0.5, 0.125, ((1, 4),)),
        "w_ret_value": normal_values(seeds[11], (D, HEADS_RET * VAL), D ** -0.5, 0.125, ((1, 4),)),
        "retain_log": draw_retain_log(jax.random.fold_in(seeds[16], 71), 0),
        "init_state": normal_values(seeds[13], (HEADS_RET, HEAD, VAL), 24.0, 144.0, ((0, 4),), jnp.float32),
        "w_out_diff": normal_values(seeds[14], (HEADS_DIFF * VAL, D), ((HEADS_DIFF + HEADS_RET) * VAL) ** -0.5, 0.125, ((0, 4),)),
        "w_out_ret": normal_values(seeds[15], (HEADS_RET * VAL, D), ((HEADS_DIFF + HEADS_RET) * VAL) ** -0.5, 0.125, ((0, 4),)),
    }


NORM_EPS = 1e-06
HEAD_EPS = 1e-05
DIFF_SCALE = 0.8
HIGHEST = lax.Precision.HIGHEST

def head_norm(values):
    return values * lax.rsqrt(lax.optimization_barrier(jnp.mean(values * values, axis=-1, keepdims=True)) + HEAD_EPS)

def diff_head(query_one, query_two, key_one, key_two, values, weight_two):
    total_rows = query_one.shape[0]
    block_rows = math.gcd(total_rows, 512)
    key_pos = jnp.arange(total_rows, dtype=jnp.int32)

    def one_block(number):
        begin_at = (number * block_rows).astype(jnp.int32)
        allowed = (begin_at + jnp.arange(block_rows, dtype=jnp.int32))[:, None] >= key_pos[None, :]

        def soft_map(query, keys):
            portion = lax.dynamic_slice_in_dim(query, begin_at, block_rows, 0)
            scores = jnp.dot(portion, keys.T, preferred_element_type=jnp.float32) * HEAD ** (-0.5)
            scores = jnp.where(allowed, scores, -jnp.inf)
            shifted = jnp.exp(scores - lax.optimization_barrier(jnp.max(scores, axis=-1, keepdims=True)))
            weighted = jnp.dot(shifted.astype(jnp.bfloat16), values, preferred_element_type=jnp.float32)
            return weighted / lax.optimization_barrier(jnp.sum(shifted, axis=-1, keepdims=True))
        return soft_map(query_one, key_one) - weight_two * soft_map(query_two, key_two)
    blocks = lax.map(one_block, jnp.arange(total_rows // block_rows, dtype=jnp.int32))
    return blocks.reshape(total_rows, VAL)

def retention(ret_query, ret_key, ret_value, retain_log, init_state):
    nblocks = TOKENS // BLOCK

    def split_blocks(data, size):
        return data.reshape(nblocks, BLOCK, HEADS_RET, size).transpose(0, 2, 1, 3)
    block_query = split_blocks(ret_query, HEAD)
    block_key = split_blocks(ret_key, HEAD)
    block_value = split_blocks(ret_value, VAL)
    log_blocks = retain_log.reshape(HEADS_RET, nblocks, BLOCK).transpose(1, 0, 2)
    sequence_index = jnp.arange(BLOCK, dtype=jnp.int32)
    causal = sequence_index[:, None] >= sequence_index[None, :]

    def ret_step(memory, inputs):
        query, keys, values, logs = inputs
        query_f = query.astype(jnp.float32)
        keys_f = keys.astype(jnp.float32)
        values_f = values.astype(jnp.float32)
        cumulative = jnp.cumsum(logs, axis=-1)
        gap_log = jnp.where(causal[None], cumulative[:, :, None] - cumulative[:, None, :], -jnp.inf)
        raw = jnp.einsum('hqd,hkd->hqk', query_f, keys_f, precision=HIGHEST)
        decayed = (raw * HEAD ** (-0.5) * jnp.exp(gap_log)).astype(jnp.bfloat16).astype(jnp.float32)
        result = jnp.einsum('hqk,hke->hqe', decayed, values_f, precision=HIGHEST)
        result = result + jnp.einsum('hqd,hde->hqe', query_f * jnp.exp(cumulative)[:, :, None], memory, precision=HIGHEST)
        last_log = cumulative[:, -1:]
        key_scaled = (keys_f * HEAD ** (-0.5) * jnp.exp(last_log - cumulative)[:, :, None]).astype(jnp.bfloat16).astype(jnp.float32)
        memory = jnp.exp(last_log)[:, :, None] * memory + jnp.einsum('hkd,hke->hde', key_scaled, values_f, precision=HIGHEST)
        return (memory, result)
    final_state, outputs = lax.scan(ret_step, init_state, (block_query, block_key, block_value, log_blocks))
    outputs = outputs.transpose(0, 2, 1, 3).reshape(TOKENS, HEADS_RET, VAL)
    return head_norm(outputs).reshape(TOKENS, HEADS_RET * VAL).astype(jnp.bfloat16)

def reference(tokens, norm_gain, w_query_one, w_query_two, w_key_one, w_key_two, w_value, mix_lambda, head_gain, w_ret_query, w_ret_key, w_ret_value, retain_log, init_state, w_out_diff, w_out_ret):
    floats = tokens.astype(jnp.float32)
    normed = (floats * lax.rsqrt(lax.optimization_barrier(jnp.mean(floats * floats, axis=-1, keepdims=True)) + NORM_EPS) * norm_gain).astype(jnp.bfloat16)

    def project(weight):
        return jnp.dot(normed, weight, preferred_element_type=jnp.float32).astype(jnp.bfloat16)
    query_one = project(w_query_one).reshape(TOKENS, HEADS_DIFF, HEAD)
    query_two = project(w_query_two).reshape(TOKENS, HEADS_DIFF, HEAD)
    key_one = project(w_key_one).reshape(TOKENS, HEADS_DIFF, HEAD)
    key_two = project(w_key_two).reshape(TOKENS, HEADS_DIFF, HEAD)
    values = project(w_value).reshape(TOKENS, HEADS_DIFF, VAL)
    head_outs = []
    for number in range(HEADS_DIFF):
        head_outs.append(diff_head(query_one[:, number], query_two[:, number], key_one[:, number], key_two[:, number], values[:, number], mix_lambda[number]))
    mixed_heads = jnp.stack(head_outs, axis=1)
    diff_out = (head_norm(mixed_heads) * head_gain * DIFF_SCALE).reshape(TOKENS, HEADS_DIFF * VAL).astype(jnp.bfloat16)
    ret_out = retention(project(w_ret_query), project(w_ret_key), project(w_ret_value), retain_log, init_state)
    total = jnp.dot(diff_out, w_out_diff, preferred_element_type=jnp.float32) + jnp.dot(ret_out, w_out_ret, preferred_element_type=jnp.float32)
    return total.astype(jnp.bfloat16)
```

```python
import functools
import math

import jax
import jax.numpy as jnp
from jax import lax
from jax.experimental import pallas as pl
from jax.experimental.pallas import tpu as pltpu
from jax.sharding import PartitionSpec as P


BLOCK = 256
NORM_EPS = 1e-06
HEAD_EPS = 1e-05
DIFF_SCALE = 0.8
HIGHEST = lax.Precision.HIGHEST
F32 = jnp.float32
BF16 = jnp.bfloat16
VMEM = pltpu.VMEM
SMEM = pltpu.SMEM
CORES = 2


def attend_kernel(
    heads, groups, halves, spans_low,
    place, lam, q_ref, kv_ref, gain_ref, o_ref,
    s_ref, m_ref, acc_ref,
):
    x, y, z, g = place[0], place[1], place[2], place[3]
    j = lax.rem(z, heads)
    rows = q_ref.shape[2]
    width = q_ref.shape[3]
    scale = (width // 2) ** (-0.5) * math.log2(math.e)
    low_half = lax.broadcasted_iota(jnp.int32, (rows, width), 1) < width // 2
    zero = jnp.zeros((rows, width), BF16)

    def slot_of(piece):
        half = lax.rem(piece, halves)
        span = piece // halves
        b = lax.rem(lax.rem(span, spans_low) - y + spans_low, spans_low)
        plane = span // spans_low
        lo, hi = lax.rem(plane, heads), plane // heads
        r = lax.rem(j - lo + heads, heads)
        d = lax.rem(lax.rem(hi + lo, groups) - g + groups, groups)
        p = lax.rem(half - x + halves, halves)
        return ((b * groups + d) * halves + p) * heads + r

    for r in range(heads):
        lo = lax.rem(j - r + heads, heads)
        hi = lax.rem(g - lo + groups * heads, groups)
        plane = hi * heads + lo
        for p in range(halves):
            last = (plane * spans_low + y) * halves + lax.rem(x + p, halves)
            q = q_ref[r, p]
            both = jnp.concatenate(
                [jnp.where(low_half, q, zero), jnp.where(low_half, zero, q)], axis=0
            )
            m_ref[...] = jnp.full(m_ref.shape, -jnp.inf, F32)

            def scores(piece):
                keys = kv_ref[slot_of(piece)][:, :width]
                return lax.dot_general(
                    both, keys, (((1,), (1,)), ((), ())), preferred_element_type=F32
                )

            def keep(piece, s):
                s_ref[piece] = s
                m = m_ref[...]
                for at in range(0, s.shape[1], 128):
                    m = jnp.maximum(m, s[:, at : at + 128])
                m_ref[...] = m

            def full(piece, carry):
                keep(piece, scores(piece))
                return carry

            lax.fori_loop(0, last, full, 0)
            s = scores(last)
            at_row = lax.rem(lax.broadcasted_iota(jnp.int32, s.shape, 0), rows)
            at_key = lax.broadcasted_iota(jnp.int32, s.shape, 1)
            keep(last, jnp.where(at_key <= at_row, s, -jnp.inf))
            peak = jnp.max(m_ref[...], axis=1, keepdims=True)
            m_ref[...] = jnp.broadcast_to(peak, m_ref.shape)
            acc_ref[...] = jnp.zeros_like(acc_ref)

            def gather(piece, carry):
                m = m_ref[...]
                s = s_ref[piece]
                e = jnp.concatenate(
                    [
                        jnp.exp2((s[:, at : at + 128] - m) * scale).astype(BF16)
                        for at in range(0, s.shape[1], 128)
                    ],
                    axis=1,
                )
                values = kv_ref[slot_of(piece)][:, width:]
                ones = jnp.ones_like(values)
                acc_ref[...] += jnp.dot(
                    e, jnp.concatenate([values, ones], axis=1), preferred_element_type=F32
                )
                return carry

            lax.fori_loop(0, last + 1, gather, 0)
            acc = acc_ref[...]
            val = acc.shape[1] // 2
            maps = acc[:, :val] / acc[:, val:]
            attn = maps[:rows] - lam[0] * maps[rows:]
            mean = jnp.mean(attn * attn, axis=-1, keepdims=True)
            out = attn * lax.rsqrt(mean + HEAD_EPS) * gain_ref[...] * DIFF_SCALE
            o_ref[r, p] = out.astype(BF16)


def attend(place, lam, q, kv, gain, heads, groups, halves, spans_low):
    slots, rows, _ = kv.shape
    full = lambda: pl.BlockSpec(memory_space=VMEM)
    return pl.pallas_call(
        functools.partial(attend_kernel, heads, groups, halves, spans_low),
        out_shape=jax.ShapeDtypeStruct((heads, halves, rows, gain.shape[-1]), BF16),
        in_specs=[
            pl.BlockSpec(memory_space=SMEM),
            pl.BlockSpec(memory_space=SMEM),
            full(), full(), full(),
        ],
        out_specs=full(),
        scratch_shapes=[
            VMEM((slots, 2 * rows, rows), F32),
            VMEM((2 * rows, 128), F32),
            VMEM((2 * rows, 2 * gain.shape[-1]), F32),
        ],
        compiler_params=pltpu.CompilerParams(vmem_limit_bytes=60 * 1024 * 1024),
        cost_estimate=pl.CostEstimate(
            flops=slots * 4 * rows * rows * 512 * 2, bytes_accessed=kv.size * 2, transcendentals=0
        ),
        name="attend",
    )(place, lam, q, kv, gain)


def lane_half(array, head, size):
    return array[:, head * size : (head + 1) * size]


def state_kernel(heads, blocks, decay, k_ref, v_ref, u_ref):
    key = k_ref.shape[1] // heads
    val = v_ref.shape[1] // heads
    for n in range(blocks):
        rows = slice(n * BLOCK, (n + 1) * BLOCK)
        for h in range(heads):
            k = lane_half(k_ref[rows, :], h, key).astype(F32)
            v = lane_half(v_ref[rows, :], h, val)
            kd = (k * key ** (-0.5) * decay[n, h]).astype(BF16)
            u_ref[n, h] = lax.dot_general(
                kd, v, (((0,), (0,)), ((), ())), preferred_element_type=F32
            )


def block_states(tail, k, v, heads, blocks):
    val = v.shape[1] // heads
    key = k.shape[1] // heads
    return pl.pallas_call(
        functools.partial(state_kernel, heads, blocks),
        out_shape=jax.ShapeDtypeStruct((blocks, heads, key, val), F32),
        in_specs=[pl.BlockSpec(memory_space=VMEM)] * 3,
        out_specs=pl.BlockSpec(memory_space=VMEM),
        cost_estimate=pl.CostEstimate(
            flops=2 * k.shape[0] * key * val * heads * 4, bytes_accessed=0, transcendentals=0
        ),
        name="block_states",
    )(tail, k, v)


def retain_kernel(heads, blocks, col_ref, row_ref, q_ref, k_ref, v_ref, s_ref, o_ref):
    key = k_ref.shape[1] // heads
    val = v_ref.shape[1] // heads
    at_row = lax.broadcasted_iota(jnp.int32, (BLOCK, BLOCK), 0)
    at_col = lax.broadcasted_iota(jnp.int32, (BLOCK, BLOCK), 1)
    causal = at_row >= at_col
    for n in range(blocks):
        rows = slice(n * BLOCK, (n + 1) * BLOCK)
        for h in range(heads):
            q = lane_half(q_ref[rows, :], h, key)
            k = lane_half(k_ref[rows, :], h, key)
            v = lane_half(v_ref[rows, :], h, val)
            c = col_ref[n, h]
            raw = lax.dot_general(q, k, (((1,), (1,)), ((), ())), preferred_element_type=F32)
            gap = jnp.where(causal, c - row_ref[n, h], -jnp.inf)
            g = (raw * key ** (-0.5) * jnp.exp(gap)).astype(BF16)
            r = jnp.dot(g, v, preferred_element_type=F32)
            r += jnp.dot(
                q.astype(F32) * jnp.exp(c), s_ref[n, h],
                precision=HIGHEST, preferred_element_type=F32,
            )
            mean = jnp.mean(r * r, axis=-1, keepdims=True)
            o_ref[rows, h * val : (h + 1) * val] = (r * lax.rsqrt(mean + HEAD_EPS)).astype(BF16)


def retain(col, row, q, k, v, states, heads, blocks):
    return pl.pallas_call(
        functools.partial(retain_kernel, heads, blocks),
        out_shape=jax.ShapeDtypeStruct(v.shape, BF16),
        in_specs=[pl.BlockSpec(memory_space=VMEM)] * 6,
        out_specs=pl.BlockSpec(memory_space=VMEM),
        cost_estimate=pl.CostEstimate(
            flops=2 * BLOCK * q.shape[0] * 1024, bytes_accessed=0, transcendentals=0
        ),
        name="retain",
    )(col, row, q, k, v, states)


def on_device(
    sp, tp,
    tokens, norm_gain, w_query_one, w_query_two, w_key_one, w_key_two, w_value, mix_lambda,
    head_gain, w_ret_query, w_ret_key, w_ret_value, retain_log, init_state, w_out_diff, w_out_ret,
):
    heads = mix_lambda.shape[0]
    ret_heads = init_state.shape[0]
    key = w_query_one.shape[1] // heads
    val = head_gain.shape[0]
    halves = tp // CORES
    planes = CORES * heads
    spans_low = sp // planes
    axes = ("sp", "tp")

    def send(array, rule):
        pairs = []
        for s in range(sp):
            for t in range(tp):
                to = rule(s // spans_low, s % spans_low, t // CORES, t % CORES)
                pairs.append((s * tp + t, (to[0] * spans_low + to[1]) * tp + to[2] * CORES + to[3]))
        return lax.ppermute(array, axes, pairs)

    s, t = lax.axis_index("sp"), lax.axis_index("tp")
    x, c = t // CORES, lax.rem(t, CORES)
    z, y = s // spans_low, lax.rem(s, spans_low)
    other_core = lambda z, y, x, c: (z, y, x, (c + 1) % CORES)

    lam_other = send(mix_lambda, other_core)
    lam_all = jnp.where(c == 0, jnp.concatenate([mix_lambda, lam_other]),
                        jnp.concatenate([lam_other, mix_lambda]))
    lam = lax.dynamic_slice_in_dim(lam_all, z, 1, 0)

    floats = tokens.astype(F32)
    normed = (
        floats * lax.rsqrt(jnp.mean(floats * floats, axis=-1, keepdims=True) + NORM_EPS) * norm_gain
    ).astype(BF16)

    pieces = []
    for h in range(heads):
        for w, size in ((w_key_one, key), (w_key_two, key), (w_value, val),
                        (w_query_one, key), (w_query_two, key)):
            pieces.append(w[:, h * size : (h + 1) * size])
    weights = jnp.concatenate(pieces + [w_ret_query, w_ret_key, w_ret_value], axis=1)
    head_cols = 4 * key + val
    attn_cols = heads * head_cols

    chip_rows = []
    for p in range(halves):
        block = normed if p == 0 else send(normed, lambda z, y, x, c: (z, y, (x - p) % halves, c))
        partner = send(block, other_core)
        chip_rows.append(
            jnp.where(c == 0, jnp.concatenate([block, partner]), jnp.concatenate([partner, block]))
        )
    half_rows = chip_rows[0].shape[0]
    row_count = half_rows * halves
    projected = [
        jnp.dot(rows, weights, preferred_element_type=F32).astype(BF16) for rows in chip_rows
    ]

    def spread(r):
        def rule(z, y, x, c):
            lo, hi = z % heads, z // heads
            return (c * heads + (lo + r) % heads, y, x, (hi + lo) % CORES)
        return rule

    def unspread(r):
        def rule(z, y, x, c):
            j = z % heads
            lo = (j - r) % heads
            hi = (c - lo) % CORES
            return (hi * heads + lo, y, x, z // heads)
        return rule

    lo_here = lax.rem(z, heads)
    own_keys, own_queries = [], []
    for p in range(halves):
        got = []
        for r in range(heads):
            which = lax.rem(lo_here + r, heads)
            message = lax.dynamic_slice_in_dim(projected[p], which * head_cols, head_cols, 1)
            got.append(send(message, spread(r)))
        own_keys.append(jnp.stack([m[:, : 2 * key + val] for m in got]))
        own_queries.append([m[:, 2 * key + val :] for m in got])
    queries = jnp.stack(
        [jnp.stack([own_queries[p][r] for p in range(halves)]) for r in range(heads)]
    )
    slots = []
    for b in range(spans_low):
        rule = lambda z, y, x, c: (z, (y - b) % spans_low, x, c)
        shifted = [k if b == 0 else send(k, rule) for k in own_keys]
        slots += shifted
        slots += [send(k, other_core) for k in shifted]
    kv = jnp.concatenate(slots, axis=0)

    blocks = row_count // BLOCK
    ret_width = ret_heads * key
    slab = jnp.zeros((row_count, projected[0].shape[1] - attn_cols), BF16)
    for p in range(halves):
        slab = lax.dynamic_update_slice_in_dim(
            slab, projected[p][:, attn_cols:], lax.rem(x + p, halves) * half_rows, 0
        )
    ret_q, ret_k, ret_v = slab[:, :ret_width], slab[:, ret_width : 2 * ret_width], slab[:, 2 * ret_width :]
    cumulative = jnp.cumsum(retain_log.reshape(ret_heads, blocks, BLOCK).transpose(1, 0, 2), axis=-1)
    last = cumulative[:, :, -1]
    tail = jnp.exp(last[:, :, None] - cumulative)[..., None]
    parts = block_states(tail, ret_k, ret_v, ret_heads, blocks)
    local = parts[0]
    for n in range(1, blocks):
        local = jnp.exp(last[n])[:, None, None] * local + parts[n]
    total_log = jnp.sum(last, axis=0)
    before, before_log = jnp.zeros_like(local), jnp.zeros_like(total_log)
    step = 1
    while step < sp:
        packed = jnp.concatenate(
            [local, jnp.broadcast_to(total_log[:, None, None], (ret_heads, 8, val))], axis=1
        )
        pairs = [(i, i ^ step) for i in range(sp)]
        heard = lax.ppermute(packed, "sp", pairs)
        state, log = heard[:, :key], heard[:, key, 0]
        upper = (s // step) % 2 == 1
        decay = lambda a: jnp.exp(a)[:, None, None]
        before = jnp.where(upper, state * decay(before_log) + before, before)
        before_log = jnp.where(upper, log + before_log, before_log)
        local = jnp.where(
            upper, state * decay(total_log) + local, local * decay(log) + state
        )
        total_log = total_log + log
        step *= 2
    carried = before + jnp.exp(before_log)[:, None, None] * init_state
    states = [carried]
    for n in range(blocks - 1):
        states.append(jnp.exp(last[n])[:, None, None] * states[-1] + parts[n])
    ret_out = retain(
        cumulative[..., None], cumulative[:, :, None, :], ret_q, ret_k, ret_v,
        jnp.stack(states), ret_heads, blocks,
    )

    place = jnp.stack([x, y, z, c]).astype(jnp.int32)
    diff = attend(place, lam, queries, kv, head_gain[None, :], heads, CORES, halves, spans_low)
    home = [send(diff[r], unspread(r)) for r in range(heads)]
    by_head = []
    for h in range(heads):
        block = home[0]
        for r in range(1, heads):
            block = jnp.where(lax.rem(lo_here + r, heads) == h, home[r], block)
        by_head.append(block)
    mine = half_rows // CORES
    result = None
    for p in reversed(range(halves)):
        ret_half = lax.dynamic_slice_in_dim(ret_out, lax.rem(x + p, halves) * half_rows, half_rows, 0)
        cols = jnp.concatenate([b[p] for b in by_head], axis=1)

        def product(core):
            a = lax.dynamic_slice_in_dim(cols, core * mine, mine, 0)
            b = lax.dynamic_slice_in_dim(ret_half, core * mine, mine, 0)
            return jnp.dot(a, w_out_diff, preferred_element_type=F32) + jnp.dot(
                b, w_out_ret, preferred_element_type=F32
            )

        away = send(product(1 - c).astype(BF16), other_core)
        summed = product(c) + away.astype(F32)
        if p > 0:
            summed = send(
                summed.astype(BF16), lambda z, y, x, c: (z, y, (x + p) % halves, c)
            ).astype(F32)
        result = summed if result is None else result + summed
    return result.astype(BF16)


def solution(mesh):
    sp, tp = mesh.shape["sp"], mesh.shape["tp"]
    in_specs = (
        P(("sp", "tp"), None), P(),
        P(None, "tp"), P(None, "tp"), P(None, "tp"), P(None, "tp"), P(None, "tp"),
        P("tp"), P(),
        P(None, "tp"), P(None, "tp"), P(None, "tp"),
        P("tp", "sp"), P("tp", None, None), P("tp", None), P("tp", None),
    )
    return jax.shard_map(
        functools.partial(on_device, sp, tp), mesh=mesh, in_specs=in_specs,
        out_specs=P(("sp", "tp"), None), check_vma=False,
    )
```

```python
import functools
import math

import jax
import jax.numpy as jnp
from jax import lax
from jax.experimental import pallas as pl
from jax.experimental.pallas import tpu as pltpu
from jax.sharding import PartitionSpec as P


BLOCK = 256
NORM_EPS = 1e-06
HEAD_EPS = 1e-05
DIFF_SCALE = 0.8
HIGHEST = lax.Precision.HIGHEST
F32 = jnp.float32
BF16 = jnp.bfloat16
VMEM = pltpu.VMEM
SMEM = pltpu.SMEM
CORES = 2


def place(spans_low):
    s, t = lax.axis_index("sp"), lax.axis_index("tp")
    return t // CORES, lax.rem(s, spans_low), s // spans_low, lax.rem(t, CORES)


def whole(count):
    return [pl.BlockSpec(memory_space=VMEM)] * count


def project_kernel(heads, spans_low, *refs):
    sources, refs = refs[:11], refs[11:]
    targets, refs = refs[: heads + 1], refs[heads + 1 :]
    staged, refs = refs[: heads + 1], refs[heads + 1 :]
    rows_ref, (*landed, sem, out_sem) = refs[0], refs[1:]
    messages, ret_ref = staged[:heads], staged[heads]
    copies = [
        pltpu.make_async_copy(source, target, sem.at[n])
        for n, (source, target) in enumerate(zip(sources, landed))
    ]
    copies[10].start()
    for copy in copies[:10]:
        copy.start()
    _, _, z, c = place(spans_low)
    mine = sources[0].shape[0]
    copies[10].wait()
    for n, core in ((0, c), (1, CORES - 1 - c)):
        copies[n].wait()
        floats = landed[n][...].astype(F32)
        mean = jnp.mean(floats * floats, axis=-1, keepdims=True)
        rows_ref[pl.ds(pl.multiple_of(core * mine, mine), mine), :] = (
            floats * lax.rsqrt(mean + NORM_EPS) * landed[10][...]
        ).astype(BF16)
    k1, k2, v, q1, q2, rq, rk, rv = range(2, 10)
    rows = rows_ref.shape[0]
    width = sources[k1].shape[1]
    size = width // heads
    lane = lax.broadcasted_iota(jnp.int32, (rows, 2 * size), 1)
    low = lax.rem(z, heads)

    def product(*which):
        for n in which:
            copies[n].wait()
        parts = [landed[n][...] for n in which]
        w = parts[0] if len(parts) == 1 else jnp.concatenate(parts, axis=1)
        return jnp.dot(rows_ref[...], w, preferred_element_type=F32)

    def side(both, h):
        one, two = both[:, :width], both[:, width:]
        a = one if h == 0 else pltpu.roll(one, width - h * size, 1)
        shift = (size - h * size) % width
        b = two if shift == 0 else pltpu.roll(two, shift, 1)
        return jnp.where(lane < size, a[:, : 2 * size], b[:, : 2 * size]).astype(BF16)

    def deal(n, per_head):
        for r in range(heads):
            chosen = per_head[r]
            for h in range(heads):
                if h != r:
                    chosen = jnp.where(lax.rem(low + r, heads) == h, per_head[h], chosen)
            messages[r][n] = chosen

    keys = product(k1, k2)
    deal(0, [side(keys, h) for h in range(heads)])
    values = product(v)
    val = values.shape[1] // heads
    deal(1, [values[:, h * val : (h + 1) * val].astype(BF16) for h in range(heads)])
    queries = product(q1, q2)
    deal(2, [side(queries, h) for h in range(heads)])
    leaving = [
        pltpu.make_async_copy(source, target, out_sem.at[n])
        for n, (source, target) in enumerate(zip(staged, targets))
    ]
    for copy in leaving[:heads]:
        copy.start()
    ret_ref[:, : 2 * width] = product(rq, rk).astype(BF16)
    ret_ref[:, 2 * width :] = product(rv).astype(BF16)
    leaving[heads].start()
    for copy in leaving:
        copy.wait()


def project(block, partner, gain, weights, heads, val, spans_low):
    mine, width = block.shape
    rows = CORES * mine
    key = weights[0].shape[1]
    ret = sum(w.shape[1] for w in weights[5:])
    message = (3, rows, val)
    return pl.pallas_call(
        functools.partial(project_kernel, heads, spans_low),
        out_shape=[jax.ShapeDtypeStruct(message, BF16)] * heads
        + [jax.ShapeDtypeStruct((rows, ret), BF16)],
        in_specs=[pl.BlockSpec(memory_space=pltpu.HBM)] * (3 + len(weights)),
        out_specs=[pl.BlockSpec(memory_space=pltpu.HBM)] * (heads + 1),
        scratch_shapes=[VMEM(message, BF16)] * heads + [VMEM((rows, ret), BF16), VMEM((rows, width), BF16)]
        + [VMEM(a.shape, a.dtype) for a in (block, partner, *weights, gain)]
        + [pltpu.SemaphoreType.DMA((3 + len(weights),)), pltpu.SemaphoreType.DMA((heads + 1,))],
        compiler_params=pltpu.CompilerParams(vmem_limit_bytes=60 << 20),
        cost_estimate=pl.CostEstimate(
            flops=2 * rows * width * (6 * key + 2 * weights[4].shape[1]) * 2,
            bytes_accessed=0, transcendentals=0,
        ),
        name="project",
    )(block, partner, *weights, gain)


def attend(own, shared, lam, lam_other, gain, heads, halves, spans_low, sp):
    rows, val = own[0].shape[1], own[0].shape[2]
    group = halves if sp * halves * halves * rows * rows * 8 <= (24 << 20) else 1
    count = len(own) + len(shared)

    def kernel(*refs):
        own_refs, shared_refs = refs[: len(own)], refs[len(own) : count]
        lam_ref, other_ref, gain_ref = refs[count : count + 3]
        outs = refs[count + 3 : count + 3 + heads]
        kv_ref, q_ref, s_ref, m_ref, acc_ref, sem = refs[count + 3 + heads :]
        x, y, z, c = place(spans_low)
        j = lax.rem(z, heads)

        def span_of(r, b, d):
            low = lax.rem(j - r + heads, heads)
            core = lax.rem(c + d, CORES)
            high = lax.rem(core - low + CORES * heads, CORES)
            return (high * heads + low) * spans_low + lax.rem(y + b, spans_low)

        copies = []

        def fetch(source, target):
            copy = pltpu.make_async_copy(source, target, sem.at[len(copies)])
            copy.start()
            copies.append(copy)

        for p in range(halves):
            half = lax.rem(x + p, halves)
            for r in range(heads):
                fetch(own_refs[p * heads + r].at[pl.ds(0, 2)], kv_ref.at[span_of(r, 0, 0), half])
                fetch(own_refs[p * heads + r].at[2], q_ref.at[r, p])
        n = 0
        for b in range(spans_low):
            for d in range(CORES):
                if b == 0 and d == 0:
                    continue
                for p in range(halves):
                    for r in range(heads):
                        fetch(
                            shared_refs[n].at[r],
                            kv_ref.at[span_of(r, b, d), lax.rem(x + p, halves)],
                        )
                    n += 1
        for copy in copies:
            copy.wait()

        owner = z // heads
        lam = lam_ref[j]
        lam = jnp.where(c == owner, lam, other_ref[j])
        scale = (val // 2) ** (-0.5) * math.log2(math.e)
        lane = lax.broadcasted_iota(jnp.int32, (rows, val), 1)
        zero = jnp.zeros((rows, val), BF16)
        keys = halves * rows

        def part(r, first):
            span = span_of(r, 0, 0)
            queries = []
            for p in range(first, first + group):
                q = q_ref[r, p]
                queries += [jnp.where(lane < val // 2, q, zero), jnp.where(lane < val // 2, zero, q)]
            stack = jnp.concatenate(queries, axis=0)
            m_ref[...] = jnp.full(m_ref.shape, -jnp.inf, F32)

            def scores(at):
                pieces = kv_ref.at[at]
                k = jnp.concatenate([pieces[h, 0] for h in range(halves)], axis=0)
                return lax.dot_general(
                    stack, k, (((1,), (1,)), ((), ())), preferred_element_type=F32
                )

            def keep(at, s):
                s_ref[at] = s
                m = m_ref[...]
                for lanes in range(0, keys, 128):
                    m = jnp.maximum(m, s[:, lanes : lanes + 128])
                m_ref[...] = m

            def full(at, carry):
                keep(at, scores(at))
                return carry

            lax.fori_loop(0, span, full, 0)
            s = scores(span)
            at_key = lax.broadcasted_iota(jnp.int32, (rows, keys), 1)
            at_row = lax.broadcasted_iota(jnp.int32, (rows, keys), 0)
            masked = []
            for p in range(group):
                begin = lax.rem(x + first + p, halves) * rows
                for i in range(2):
                    at = (2 * p + i) * rows
                    masked.append(jnp.where(at_key <= at_row + begin, s[at : at + rows], -jnp.inf))
            keep(span, jnp.concatenate(masked, axis=0))
            m_ref[...] = jnp.broadcast_to(
                jnp.max(m_ref[...], axis=1, keepdims=True), m_ref.shape
            )
            acc_ref[...] = jnp.zeros_like(acc_ref)
            ones = jnp.ones((keys, val), BF16)

            def gather(at, carry):
                m = m_ref[...]
                s = s_ref[at]
                e = jnp.concatenate(
                    [
                        jnp.exp2((s[:, lanes : lanes + 128] - m) * scale).astype(BF16)
                        for lanes in range(0, keys, 128)
                    ],
                    axis=1,
                )
                pieces = kv_ref.at[at]
                v = jnp.concatenate([pieces[h, 1] for h in range(halves)], axis=0)
                acc_ref[...] += jnp.dot(
                    e, jnp.concatenate([v, ones], axis=1), preferred_element_type=F32
                )
                return carry

            lax.fori_loop(0, span + 1, gather, 0)
            for p in range(group):
                at = 2 * p * rows
                one, two = acc_ref[at : at + rows], acc_ref[at + rows : at + 2 * rows]
                attn = one[:, :val] / one[:, val:] - lam * (two[:, :val] / two[:, val:])
                mean = jnp.mean(attn * attn, axis=-1, keepdims=True)
                out = attn * lax.rsqrt(mean + HEAD_EPS) * gain_ref[...] * DIFF_SCALE
                outs[r][first + p] = out.astype(BF16)

        for r in range(heads):
            for first in range(0, halves, group):
                part(r, first)

    total = 2 * group * rows
    fetches = 2 * halves * heads + len(shared) * heads
    return pl.pallas_call(
        kernel,
        out_shape=[jax.ShapeDtypeStruct((halves, rows, val), BF16)] * heads,
        in_specs=[pl.BlockSpec(memory_space=pltpu.HBM)] * count
        + [pl.BlockSpec(memory_space=SMEM)] * 2 + whole(1),
        out_specs=whole(heads),
        scratch_shapes=[
            VMEM((sp, halves, 2, rows, val), BF16),
            VMEM((heads, halves, rows, val), BF16),
            VMEM((sp, total, halves * rows), F32),
            VMEM((total, 128), F32),
            VMEM((total, 2 * val), F32),
            pltpu.SemaphoreType.DMA((fetches,)),
        ],
        compiler_params=pltpu.CompilerParams(vmem_limit_bytes=60 * 1024 * 1024),
        cost_estimate=pl.CostEstimate(
            flops=heads * halves * rows * sp * rows * val * 16, bytes_accessed=0, transcendentals=0
        ),
        name="attend",
    )(*own, *shared, lam, lam_other, gain)


def running_log(logs, column):
    size = logs.shape[1]
    row = lax.broadcasted_iota(jnp.int32, (size, size), 0)
    col = lax.broadcasted_iota(jnp.int32, (size, size), 1)
    if column:
        upto = (col <= row).astype(F32)
        return lax.dot_general(
            upto, logs, (((1,), (1,)), ((), ())), precision=HIGHEST, preferred_element_type=F32
        )
    upto = (row <= col).astype(F32)
    return jnp.dot(logs, upto, precision=HIGHEST, preferred_element_type=F32)


def retention_states(slabs, logs, heads, key, val, spans_low):
    halves = len(slabs)
    rows, width = slabs[0].shape
    blocks = halves * rows // BLOCK

    def kernel(log_ref, *refs):
        slab_refs, (out_ref, u_ref, slab_ref) = refs[:halves], refs[halves:]
        x, _, _, _ = place(spans_low)
        for p in range(halves):
            begin = lax.rem(x + p, halves) * rows
            slab_ref[pl.ds(pl.multiple_of(begin, rows), rows), :] = slab_refs[p][...]
        for h in range(heads):
            state, total = None, None
            for n in range(blocks):
                at = slice(n * BLOCK, (n + 1) * BLOCK)
                k = slab_ref[at, (heads + h) * key : (heads + h + 1) * key].astype(F32)
                v = slab_ref[at, 2 * heads * key + h * val : 2 * heads * key + (h + 1) * val]
                logs = log_ref[h : h + 1, at]
                c_col = running_log(logs, True)
                last = jnp.sum(logs, axis=1, keepdims=True)
                kd = (k * key ** (-0.5) * jnp.exp(last - c_col)).astype(BF16)
                u = lax.dot_general(
                    kd, v, (((0,), (0,)), ((), ())), preferred_element_type=F32
                )
                u_ref[n, h] = u
                state = u if n == 0 else state * jnp.exp(last) + u
                total = last if n == 0 else total + last
            out_ref[h, :key] = state
            out_ref[h, key:] = jnp.broadcast_to(total, (8, val))

    return pl.pallas_call(
        kernel,
        out_shape=[
            jax.ShapeDtypeStruct((heads, key + 8, val), F32),
            jax.ShapeDtypeStruct((blocks, heads, key, val), F32),
        ],
        in_specs=whole(1 + halves),
        out_specs=whole(2),
        scratch_shapes=[VMEM((halves * rows, width), BF16)],
        cost_estimate=pl.CostEstimate(
            flops=2 * halves * rows * key * val * heads * 8, bytes_accessed=0, transcendentals=0
        ),
        name="states",
    )(logs, *slabs)


def retain(slabs, logs, parts, before, init, heads, key, val, spans_low):
    halves = len(slabs)
    rows, width = slabs[0].shape
    per_half = rows // BLOCK

    def kernel(log_ref, parts_ref, before_ref, init_ref, *refs):
        slab_refs, (out_ref, slab_ref) = refs[:halves], refs[halves:]
        x, _, _, _ = place(spans_low)
        for p in range(halves):
            begin = lax.rem(x + p, halves) * rows
            slab_ref[pl.ds(pl.multiple_of(begin, rows), rows), :] = slab_refs[p][...]
        at_row = lax.broadcasted_iota(jnp.int32, (BLOCK, BLOCK), 0)
        at_col = lax.broadcasted_iota(jnp.int32, (BLOCK, BLOCK), 1)
        for h in range(heads):
            state = before_ref[h, :key] + jnp.exp(before_ref[h, key : key + 1]) * init_ref[h]
            for n in range(halves * per_half):
                at = slice(n * BLOCK, (n + 1) * BLOCK)
                q = slab_ref[at, h * key : (h + 1) * key]
                k = slab_ref[at, (heads + h) * key : (heads + h + 1) * key]
                v = slab_ref[at, 2 * heads * key + h * val : 2 * heads * key + (h + 1) * val]
                logs = log_ref[h : h + 1, at]
                c_col = running_log(logs, True)
                c_row = running_log(logs, False)
                raw = lax.dot_general(q, k, (((1,), (1,)), ((), ())), preferred_element_type=F32)
                gap = jnp.where(at_row >= at_col, c_col - c_row, -jnp.inf)
                g = (raw * key ** (-0.5) * jnp.exp(gap)).astype(BF16)
                r = jnp.dot(g, v, preferred_element_type=F32)
                r += jnp.dot(
                    q.astype(F32) * jnp.exp(c_col), state,
                    precision=HIGHEST, preferred_element_type=F32,
                )
                mean = jnp.mean(r * r, axis=-1, keepdims=True)
                p = lax.rem(n // per_half - x + halves, halves)
                inside = slice((n % per_half) * BLOCK, (n % per_half + 1) * BLOCK)
                out_ref[p, inside, h * val : (h + 1) * val] = (
                    r * lax.rsqrt(mean + HEAD_EPS)
                ).astype(BF16)
                last = jnp.sum(logs, axis=1, keepdims=True)
                state = state * jnp.exp(last) + parts_ref[n, h]

    return pl.pallas_call(
        kernel,
        out_shape=jax.ShapeDtypeStruct((halves, rows, heads * val), BF16),
        in_specs=whole(4 + halves),
        out_specs=pl.BlockSpec(memory_space=VMEM),
        scratch_shapes=[VMEM((halves * rows, width), BF16)],
        cost_estimate=pl.CostEstimate(
            flops=2 * BLOCK * halves * rows * 1024, bytes_accessed=0, transcendentals=0
        ),
        name="retain",
    )(logs, parts, before, init, *slabs)


def on_device(
    sp, tp,
    tokens, norm_gain, w_query_one, w_query_two, w_key_one, w_key_two, w_value, mix_lambda,
    head_gain, w_ret_query, w_ret_key, w_ret_value, retain_log, init_state, w_out_diff, w_out_ret,
):
    heads = mix_lambda.shape[0]
    ret_heads = init_state.shape[0]
    key = init_state.shape[1]
    val = head_gain.shape[0]
    halves = tp // CORES
    spans_low = sp // (CORES * heads)
    axes = ("sp", "tp")

    def send(array, rule):
        pairs = []
        for s in range(sp):
            for t in range(tp):
                to = rule(s // spans_low, s % spans_low, t // CORES, t % CORES)
                pairs.append((s * tp + t, (to[0] * spans_low + to[1]) * tp + to[2] * CORES + to[3]))
        return lax.ppermute(array, axes, pairs)

    _, _, z, c = place(spans_low)
    s = lax.axis_index("sp")
    other_core = lambda z, y, x, c: (z, y, x, (c + 1) % CORES)

    weights = (
        w_key_one, w_key_two, w_value, w_query_one, w_query_two,
        w_ret_query, w_ret_key, w_ret_value,
    )
    blocks = [tokens] + [
        send(tokens, lambda z, y, x, c: (z, y, (x - p) % halves, c)) for p in range(1, halves)
    ]
    lam_other = send(mix_lambda, other_core)

    after = lambda value, event: lax.optimization_barrier((value, event))[0]

    def fetch(weight, event):
        return [weight] + [
            send(after(weight, event), lambda z, y, x, c: (z, y, (x - q) % halves, c))
            for q in range(1, halves)
        ]

    def spread(r):
        def rule(z, y, x, c):
            lo, hi = z % heads, z // heads
            return (c * heads + (lo + r) % heads, y, x, (hi + lo) % CORES)

        return rule

    def unspread(r):
        def rule(z, y, x, c):
            j = z % heads
            lo = (j - r) % heads
            hi = (c - lo) % CORES
            return (hi * heads + lo, y, x, z // heads)

        return rule

    own, slabs = [], []
    for block in blocks:
        block = after(block, slabs[-1]) if slabs else block
        partner = send(block, other_core)
        *messages, slab = project(
            block, partner, norm_gain[None, :], weights, heads, val, spans_low
        )
        own.append([send(message, spread(r)) for r, message in enumerate(messages)])
        slabs.append(slab)
    half_rows = slabs[0].shape[0]
    w_diff = fetch(w_out_diff, slabs[0])
    w_ret = fetch(w_out_ret, slabs[-1])

    shared, packs = {}, []
    for p in range(halves):
        arrived = own[p] if p == halves - 1 else after(own[p], slabs[p + 1])
        kv = jnp.stack([message[:2] for message in arrived])
        packs.append(kv)
        for b in range(spans_low):
            moved = kv if b == 0 else send(kv, lambda z, y, x, c: (z, (y - b) % spans_low, x, c))
            if b:
                shared[b, 0, p] = moved
            shared[b, 1, p] = send(moved, other_core)
    shared = [
        shared[b, d, p]
        for b in range(spans_low) for d in range(CORES) for p in range(halves) if b or d
    ]

    slabs = after(slabs, packs[0])
    local, parts = retention_states(slabs, retain_log, ret_heads, key, val, spans_low)
    before = jnp.zeros_like(local)
    is_state = lax.broadcasted_iota(jnp.int32, local.shape, 1) < key

    def join(first, second):
        return first * jnp.where(is_state, jnp.exp(second[:, key : key + 1]), 1.0) + second

    diff = attend(
        [message for half in own for message in half], shared, mix_lambda, lam_other,
        head_gain[None, :], heads, halves, spans_low, sp,
    )
    step = 1
    while step < sp:
        heard = lax.ppermute(local, "sp", [(i, i ^ step) for i in range(sp)])
        if step == 1:
            heard = after(heard, packs[-1])
        if 2 * step >= sp:
            heard = after(heard, diff)
        upper = (s // step) % 2 == 1
        before = jnp.where(upper, join(heard, before), before)
        local = jnp.where(upper, join(heard, local), join(local, heard))
        step *= 2
    ret_out = retain(slabs, retain_log, parts, before, init_state, ret_heads, key, val, spans_low)

    home = [send(diff[r], unspread(r)) for r in range(heads)]
    low = lax.rem(z, heads)
    by_head = []
    for h in range(heads):
        block = home[0]
        for r in range(1, heads):
            block = jnp.where(lax.rem(low + r, heads) == h, home[r], block)
        by_head.append(block)
    mine = half_rows // CORES
    across = lambda p: lambda z, y, x, c: (z, y, (x + p) % halves, c)
    rows_of = lambda a, core: lax.dynamic_slice_in_dim(a, core * mine, mine, 0)

    def product(a, w):
        return jnp.dot(a, w, preferred_element_type=F32)

    w_diff = [(w, send(after(w, packs[-1]), other_core)) for w in w_diff]
    w_ret = [(w, send(after(w, diff), other_core)) for w in w_ret]
    result = None
    for p in reversed(range(halves)):
        cols = jnp.concatenate([b[p] for b in by_head] + [ret_out[p]], axis=1)
        if p:
            cols = send(cols, across(p))
        theirs = send(rows_of(cols, 1 - c), other_core)
        q = (halves - p) % halves
        split = heads * val
        for core, rows in enumerate((rows_of(cols, c), theirs)):
            term = product(rows[:, :split], w_diff[q][core]) + product(rows[:, split:], w_ret[q][core])
            result = term if result is None else result + term
    return result.astype(BF16)


def solution(mesh):
    sp, tp = mesh.shape["sp"], mesh.shape["tp"]
    in_specs = (
        P(("sp", "tp"), None), P(),
        P(None, "tp"), P(None, "tp"), P(None, "tp"), P(None, "tp"), P(None, "tp"),
        P("tp"), P(),
        P(None, "tp"), P(None, "tp"), P(None, "tp"),
        P("tp", "sp"), P("tp", None, None), P("tp", None), P("tp", None),
    )

    def body(*args):
        return on_device(sp, tp, *args)

    return jax.shard_map(
        body, mesh=mesh, in_specs=in_specs, out_specs=P(("sp", "tp"), None), check_vma=False
    )
```

```python
import functools
import math

import jax
import jax.numpy as jnp
from jax import lax
from jax.experimental import pallas as pl
from jax.experimental.pallas import tpu as pltpu
from jax.sharding import PartitionSpec as P


BLOCK = 256
NORM_EPS = 1e-06
HEAD_EPS = 1e-05
DIFF_SCALE = 0.8
HIGHEST = lax.Precision.HIGHEST
F32 = jnp.float32
BF16 = jnp.bfloat16
VMEM = pltpu.VMEM
SMEM = pltpu.SMEM
CORES = 2


def place(spans_low):
    s, t = lax.axis_index("sp"), lax.axis_index("tp")
    return t // CORES, lax.rem(s, spans_low), s // spans_low, lax.rem(t, CORES)


def whole(count):
    return [pl.BlockSpec(memory_space=VMEM)] * count


def project_kernel(heads, spans_low, *refs):
    sources, refs = refs[:11], refs[11:]
    targets, refs = refs[: heads + 1], refs[heads + 1 :]
    staged, refs = refs[: heads + 1], refs[heads + 1 :]
    rows_ref, (*landed, sem, out_sem) = refs[0], refs[1:]
    messages, ret_ref = staged[:heads], staged[heads]
    copies = [
        pltpu.make_async_copy(source, target, sem.at[n])
        for n, (source, target) in enumerate(zip(sources, landed))
    ]
    copies[10].start()
    for copy in copies[:10]:
        copy.start()
    _, _, z, c = place(spans_low)
    mine = sources[0].shape[0]
    copies[10].wait()
    for n, core in ((0, c), (1, CORES - 1 - c)):
        copies[n].wait()
        floats = landed[n][...].astype(F32)
        mean = jnp.mean(floats * floats, axis=-1, keepdims=True)
        rows_ref[pl.ds(pl.multiple_of(core * mine, mine), mine), :] = (
            floats * lax.rsqrt(mean + NORM_EPS) * landed[10][...]
        ).astype(BF16)
    k1, k2, v, q1, q2, rq, rk, rv = range(2, 10)
    rows = rows_ref.shape[0]
    width = sources[k1].shape[1]
    size = width // heads
    lane = lax.broadcasted_iota(jnp.int32, (rows, 2 * size), 1)
    low = lax.rem(z, heads)

    def product(*which):
        for n in which:
            copies[n].wait()
        parts = [landed[n][...] for n in which]
        w = parts[0] if len(parts) == 1 else jnp.concatenate(parts, axis=1)
        return jnp.dot(rows_ref[...], w, preferred_element_type=F32)

    def side(both, h):
        one, two = both[:, :width], both[:, width:]
        a = one if h == 0 else pltpu.roll(one, width - h * size, 1)
        shift = (size - h * size) % width
        b = two if shift == 0 else pltpu.roll(two, shift, 1)
        return jnp.where(lane < size, a[:, : 2 * size], b[:, : 2 * size]).astype(BF16)

    def deal(n, per_head):
        for r in range(heads):
            chosen = per_head[r]
            for h in range(heads):
                if h != r:
                    chosen = jnp.where(lax.rem(low + r, heads) == h, per_head[h], chosen)
            messages[r][n] = chosen

    keys = product(k1, k2)
    deal(0, [side(keys, h) for h in range(heads)])
    values = product(v)
    val = values.shape[1] // heads
    deal(1, [values[:, h * val : (h + 1) * val].astype(BF16) for h in range(heads)])
    queries = product(q1, q2)
    deal(2, [side(queries, h) for h in range(heads)])
    leaving = [
        pltpu.make_async_copy(source, target, out_sem.at[n])
        for n, (source, target) in enumerate(zip(staged, targets))
    ]
    for copy in leaving[:heads]:
        copy.start()
    ret_ref[:, : 2 * width] = product(rq, rk).astype(BF16)
    ret_ref[:, 2 * width :] = product(rv).astype(BF16)
    leaving[heads].start()
    for copy in leaving:
        copy.wait()


def project(block, partner, gain, weights, heads, val, spans_low):
    mine, width = block.shape
    rows = CORES * mine
    key = weights[0].shape[1]
    ret = sum(w.shape[1] for w in weights[5:])
    message = (3, rows, val)
    return pl.pallas_call(
        functools.partial(project_kernel, heads, spans_low),
        out_shape=[jax.ShapeDtypeStruct(message, BF16)] * heads
        + [jax.ShapeDtypeStruct((rows, ret), BF16)],
        in_specs=[pl.BlockSpec(memory_space=pltpu.HBM)] * (3 + len(weights)),
        out_specs=[pl.BlockSpec(memory_space=pltpu.HBM)] * (heads + 1),
        scratch_shapes=[VMEM(message, BF16)] * heads + [VMEM((rows, ret), BF16), VMEM((rows, width), BF16)]
        + [VMEM(a.shape, a.dtype) for a in (block, partner, *weights, gain)]
        + [pltpu.SemaphoreType.DMA((3 + len(weights),)), pltpu.SemaphoreType.DMA((heads + 1,))],
        compiler_params=pltpu.CompilerParams(vmem_limit_bytes=60 << 20),
        cost_estimate=pl.CostEstimate(
            flops=2 * rows * width * (6 * key + 2 * weights[4].shape[1]) * 2,
            bytes_accessed=0, transcendentals=0,
        ),
        name="project",
    )(block, partner, *weights, gain)


def attend(own, shared, lam, lam_other, gain, heads, halves, spans_low, sp):
    rows, val = own[0].shape[1], own[0].shape[2]
    group = halves if sp * halves * halves * rows * rows * 8 <= (24 << 20) else 1
    count = len(own) + len(shared)

    def kernel(*refs):
        own_refs, shared_refs = refs[: len(own)], refs[len(own) : count]
        lam_ref, other_ref, gain_ref = refs[count : count + 3]
        outs = refs[count + 3 : count + 3 + heads]
        kv_ref, q_ref, s_ref, m_ref, acc_ref, sem = refs[count + 3 + heads :]
        x, y, z, c = place(spans_low)
        j = lax.rem(z, heads)

        def span_of(r, b, d):
            low = lax.rem(j - r + heads, heads)
            core = lax.rem(c + d, CORES)
            high = lax.rem(core - low + CORES * heads, CORES)
            return (high * heads + low) * spans_low + lax.rem(y + b, spans_low)

        asked = []

        def fetch(source, span, half):
            at = span * halves + half
            pltpu.make_async_copy(source, kv_ref.at[span, half], sem.at[at]).start()

        def arrive(span):
            for half in range(halves):
                pltpu.make_async_copy(
                    kv_ref.at[span, half], kv_ref.at[span, half], sem.at[span * halves + half]
                ).wait()

        for p in range(halves):
            half = lax.rem(x + p, halves)
            for r in range(heads):
                copy = pltpu.make_async_copy(
                    own_refs[p * heads + r].at[2], q_ref.at[r, p],
                    sem.at[sp * halves + p * heads + r],
                )
                copy.start()
                asked.append(copy)
                fetch(own_refs[p * heads + r].at[pl.ds(0, 2)], span_of(r, 0, 0), half)
        n = 0
        for b in range(spans_low):
            for d in range(CORES):
                if b == 0 and d == 0:
                    continue
                for p in range(halves):
                    for r in range(heads):
                        fetch(shared_refs[n].at[r], span_of(r, b, d), lax.rem(x + p, halves))
                    n += 1
        for copy in asked:
            copy.wait()

        owner = z // heads
        lam = lam_ref[j]
        lam = jnp.where(c == owner, lam, other_ref[j])
        scale = (val // 2) ** (-0.5) * math.log2(math.e)
        lane = lax.broadcasted_iota(jnp.int32, (rows, val), 1)
        zero = jnp.zeros((rows, val), BF16)
        keys = halves * rows

        def part(r, first):
            span = span_of(r, 0, 0)
            queries = []
            for p in range(first, first + group):
                q = q_ref[r, p]
                queries += [jnp.where(lane < val // 2, q, zero), jnp.where(lane < val // 2, zero, q)]
            stack = jnp.concatenate(queries, axis=0)
            m_ref[...] = jnp.full(m_ref.shape, -jnp.inf, F32)

            def scores(at):
                pieces = kv_ref.at[at]
                k = jnp.concatenate([pieces[h, 0] for h in range(halves)], axis=0)
                return scale * lax.dot_general(
                    stack, k, (((1,), (1,)), ((), ())), preferred_element_type=F32
                )

            def keep(at, s):
                s_ref[at] = s
                m = m_ref[...]
                for lanes in range(0, keys, 128):
                    m = jnp.maximum(m, s[:, lanes : lanes + 128])
                m_ref[...] = m

            opening = r == 0 and first == 0

            def full(at, carry):
                if opening:
                    arrive(at)
                keep(at, scores(at))
                return carry

            def rest(at, carry):
                arrive(at)
                return carry

            lax.fori_loop(0, span, full, 0)
            if opening:
                lax.fori_loop(span, sp, rest, 0)
            s = scores(span)
            at_key = lax.broadcasted_iota(jnp.int32, (rows, keys), 1)
            at_row = lax.broadcasted_iota(jnp.int32, (rows, keys), 0)
            masked = []
            for p in range(group):
                begin = lax.rem(x + first + p, halves) * rows
                for i in range(2):
                    at = (2 * p + i) * rows
                    masked.append(jnp.where(at_key <= at_row + begin, s[at : at + rows], -jnp.inf))
            keep(span, jnp.concatenate(masked, axis=0))
            m_ref[...] = jnp.broadcast_to(
                jnp.max(m_ref[...], axis=1, keepdims=True), m_ref.shape
            )
            acc_ref[...] = jnp.zeros_like(acc_ref)
            ones = jnp.ones((keys, val), BF16)

            def gather(at, carry):
                m = m_ref[...]
                s = s_ref[at]
                e = jnp.concatenate(
                    [
                        jnp.exp2(s[:, lanes : lanes + 128] - m).astype(BF16)
                        for lanes in range(0, keys, 128)
                    ],
                    axis=1,
                )
                pieces = kv_ref.at[at]
                v = jnp.concatenate([pieces[h, 1] for h in range(halves)], axis=0)
                acc_ref[...] += jnp.dot(
                    e, jnp.concatenate([v, ones], axis=1), preferred_element_type=F32
                )
                return carry

            lax.fori_loop(0, span + 1, gather, 0)
            for p in range(group):
                at = 2 * p * rows
                one, two = acc_ref[at : at + rows], acc_ref[at + rows : at + 2 * rows]
                attn = one[:, :val] / one[:, val:] - lam * (two[:, :val] / two[:, val:])
                mean = jnp.mean(attn * attn, axis=-1, keepdims=True)
                out = attn * lax.rsqrt(mean + HEAD_EPS) * gain_ref[...] * DIFF_SCALE
                outs[r][first + p] = out.astype(BF16)

        for r in range(heads):
            for first in range(0, halves, group):
                part(r, first)

    total = 2 * group * rows
    fetches = sp * halves + halves * heads
    return pl.pallas_call(
        kernel,
        out_shape=[jax.ShapeDtypeStruct((halves, rows, val), BF16)] * heads,
        in_specs=[pl.BlockSpec(memory_space=pltpu.HBM)] * count
        + [pl.BlockSpec(memory_space=SMEM)] * 2 + whole(1),
        out_specs=whole(heads),
        scratch_shapes=[
            VMEM((sp, halves, 2, rows, val), BF16),
            VMEM((heads, halves, rows, val), BF16),
            VMEM((sp, total, halves * rows), F32),
            VMEM((total, 128), F32),
            VMEM((total, 2 * val), F32),
            pltpu.SemaphoreType.DMA((fetches,)),
        ],
        compiler_params=pltpu.CompilerParams(
            vmem_limit_bytes=min(60 << 20, (12 << 20) + sp * rows * halves * (total + val) * 4)
        ),
        cost_estimate=pl.CostEstimate(
            flops=heads * halves * rows * sp * rows * val * 16, bytes_accessed=0, transcendentals=0
        ),
        name="attend",
    )(*own, *shared, lam, lam_other, gain)


def running_logs(log_ref, heads, blocks, rows_too):
    logs = jnp.concatenate(
        [log_ref[h : h + 1, n * BLOCK : (n + 1) * BLOCK] for h in range(heads) for n in range(blocks)],
        axis=0,
    )
    row = lax.broadcasted_iota(jnp.int32, (BLOCK, BLOCK), 0)
    col = lax.broadcasted_iota(jnp.int32, (BLOCK, BLOCK), 1)
    columns = lax.dot_general(
        (col <= row).astype(F32), logs, (((1,), (1,)), ((), ())),
        precision=HIGHEST, preferred_element_type=F32,
    )
    if not rows_too:
        return logs, columns, None
    return logs, columns, jnp.dot(
        logs, (row <= col).astype(F32), precision=HIGHEST, preferred_element_type=F32
    )


def retention_states(slabs, logs, heads, key, val, spans_low):
    halves = len(slabs)
    rows, width = slabs[0].shape
    blocks = halves * rows // BLOCK

    def kernel(log_ref, *refs):
        slab_refs, (out_ref, u_ref, slab_ref) = refs[:halves], refs[halves:]
        x, _, _, _ = place(spans_low)
        for p in range(halves):
            begin = lax.rem(x + p, halves) * rows
            slab_ref[pl.ds(pl.multiple_of(begin, rows), rows), :] = slab_refs[p][...]
        all_logs, columns, _ = running_logs(log_ref, heads, blocks, False)
        for h in range(heads):
            state, total = None, None
            for n in range(blocks):
                at = slice(n * BLOCK, (n + 1) * BLOCK)
                k = slab_ref[at, (heads + h) * key : (heads + h + 1) * key].astype(F32)
                v = slab_ref[at, 2 * heads * key + h * val : 2 * heads * key + (h + 1) * val]
                i = h * blocks + n
                logs = all_logs[i : i + 1]
                c_col = columns[:, i : i + 1]
                last = jnp.sum(logs, axis=1, keepdims=True)
                kd = (k * key ** (-0.5) * jnp.exp(last - c_col)).astype(BF16)
                u = lax.dot_general(
                    kd, v, (((0,), (0,)), ((), ())), preferred_element_type=F32
                )
                u_ref[n, h] = u
                state = u if n == 0 else state * jnp.exp(last) + u
                total = last if n == 0 else total + last
            out_ref[h, :key] = state
            out_ref[h, key:] = jnp.broadcast_to(total, (8, val))

    return pl.pallas_call(
        kernel,
        out_shape=[
            jax.ShapeDtypeStruct((heads, key + 8, val), F32),
            jax.ShapeDtypeStruct((blocks, heads, key, val), F32),
        ],
        in_specs=whole(1 + halves),
        out_specs=whole(2),
        scratch_shapes=[VMEM((halves * rows, width), BF16)],
        cost_estimate=pl.CostEstimate(
            flops=2 * halves * rows * key * val * heads * 8, bytes_accessed=0, transcendentals=0
        ),
        name="states",
    )(logs, *slabs)


def retain(slabs, logs, parts, before, init, heads, key, val, spans_low):
    halves = len(slabs)
    rows, width = slabs[0].shape
    per_half = rows // BLOCK

    def kernel(log_ref, parts_ref, before_ref, init_ref, *refs):
        slab_refs, outs, (slab_ref, out_ref) = refs[:halves], refs[halves : 2 * halves], refs[2 * halves :]
        x, _, _, _ = place(spans_low)
        for p in range(halves):
            begin = lax.rem(x + p, halves) * rows
            slab_ref[pl.ds(pl.multiple_of(begin, rows), rows), :] = slab_refs[p][...]
        at_row = lax.broadcasted_iota(jnp.int32, (BLOCK, BLOCK), 0)
        at_col = lax.broadcasted_iota(jnp.int32, (BLOCK, BLOCK), 1)
        all_logs, columns, lines = running_logs(log_ref, heads, halves * per_half, True)
        for h in range(heads):
            state = before_ref[h, :key] + jnp.exp(before_ref[h, key : key + 1]) * init_ref[h]
            for n in range(halves * per_half):
                at = slice(n * BLOCK, (n + 1) * BLOCK)
                q = slab_ref[at, h * key : (h + 1) * key]
                k = slab_ref[at, (heads + h) * key : (heads + h + 1) * key]
                v = slab_ref[at, 2 * heads * key + h * val : 2 * heads * key + (h + 1) * val]
                i = h * halves * per_half + n
                logs = all_logs[i : i + 1]
                c_col, c_row = columns[:, i : i + 1], lines[i : i + 1]
                raw = lax.dot_general(q, k, (((1,), (1,)), ((), ())), preferred_element_type=F32)
                gap = jnp.where(at_row >= at_col, c_col - c_row, -jnp.inf)
                g = (raw * key ** (-0.5) * jnp.exp(gap)).astype(BF16)
                r = jnp.dot(g, v, preferred_element_type=F32)
                r += jnp.dot(
                    q.astype(F32) * jnp.exp(c_col), state,
                    precision=HIGHEST, preferred_element_type=F32,
                )
                mean = jnp.mean(r * r, axis=-1, keepdims=True)
                p = lax.rem(n // per_half - x + halves, halves)
                inside = slice((n % per_half) * BLOCK, (n % per_half + 1) * BLOCK)
                out_ref[p, inside, h * val : (h + 1) * val] = (
                    r * lax.rsqrt(mean + HEAD_EPS)
                ).astype(BF16)
                last = jnp.sum(logs, axis=1, keepdims=True)
                state = state * jnp.exp(last) + parts_ref[n, h]
        for p in range(halves):
            outs[p][...] = out_ref[p]

    return pl.pallas_call(
        kernel,
        out_shape=[jax.ShapeDtypeStruct((rows, heads * val), BF16)] * halves,
        in_specs=whole(4 + halves),
        out_specs=whole(halves),
        scratch_shapes=[
            VMEM((halves * rows, width), BF16), VMEM((halves, rows, heads * val), BF16)
        ],
        cost_estimate=pl.CostEstimate(
            flops=2 * BLOCK * halves * rows * 1024, bytes_accessed=0, transcendentals=0
        ),
        name="retain",
    )(logs, parts, before, init, *slabs)


def on_device(
    sp, tp,
    tokens, norm_gain, w_query_one, w_query_two, w_key_one, w_key_two, w_value, mix_lambda,
    head_gain, w_ret_query, w_ret_key, w_ret_value, retain_log, init_state, w_out_diff, w_out_ret,
):
    heads = mix_lambda.shape[0]
    ret_heads = init_state.shape[0]
    key = init_state.shape[1]
    val = head_gain.shape[0]
    halves = tp // CORES
    spans_low = sp // (CORES * heads)
    axes = ("sp", "tp")

    def send(array, rule):
        pairs = []
        for s in range(sp):
            for t in range(tp):
                to = rule(s // spans_low, s % spans_low, t // CORES, t % CORES)
                pairs.append((s * tp + t, (to[0] * spans_low + to[1]) * tp + to[2] * CORES + to[3]))
        return lax.ppermute(array, axes, pairs)

    _, _, z, c = place(spans_low)
    s = lax.axis_index("sp")
    other_core = lambda z, y, x, c: (z, y, x, (c + 1) % CORES)

    weights = (
        w_key_one, w_key_two, w_value, w_query_one, w_query_two,
        w_ret_query, w_ret_key, w_ret_value,
    )
    blocks = [tokens] + [
        send(tokens, lambda z, y, x, c: (z, y, (x - p) % halves, c)) for p in range(1, halves)
    ]
    lam_other = send(mix_lambda, other_core)

    after = lambda value, event: lax.optimization_barrier((value, event))[0]

    def fetch(weight, event):
        return [weight] + [
            send(after(weight, event), lambda z, y, x, c: (z, y, (x - q) % halves, c))
            for q in range(1, halves)
        ]

    def spread(r):
        def rule(z, y, x, c):
            lo, hi = z % heads, z // heads
            return (c * heads + (lo + r) % heads, y, x, (hi + lo) % CORES)

        return rule

    def unspread(r):
        def rule(z, y, x, c):
            j = z % heads
            lo = (j - r) % heads
            hi = (c - lo) % CORES
            return (hi * heads + lo, y, x, z // heads)

        return rule

    own, slabs = [], []
    for block in blocks:
        block = after(block, slabs[-1]) if slabs else block
        partner = send(block, other_core)
        *messages, slab = project(
            block, partner, norm_gain[None, :], weights, heads, val, spans_low
        )
        own.append([send(message, spread(r)) for r, message in enumerate(messages)])
        slabs.append(slab)
    half_rows = slabs[0].shape[0]
    w_out = fetch(jnp.concatenate([w_out_diff, w_out_ret]), slabs[0])

    shared, packs = {}, []
    for p in range(halves):
        arrived = own[p] if p == halves - 1 else after(own[p], slabs[p + 1])
        kv = jnp.stack([message[:2] for message in arrived])
        packs.append(kv)
        for b in range(spans_low):
            moved = kv
            if b:
                moved = send(kv, lambda z, y, x, c: (z, (y - b) % spans_low, x, c))
                shared[b, 0, p] = moved
            shared[b, 1, p] = send(moved, other_core)
    shared = [
        shared[b, d, p]
        for b in range(spans_low) for d in range(CORES) for p in range(halves) if b or d
    ]

    slabs = after(slabs, packs[0])
    local, parts = retention_states(slabs, retain_log, ret_heads, key, val, spans_low)
    before = jnp.zeros_like(local)
    is_state = lax.broadcasted_iota(jnp.int32, local.shape, 1) < key

    def join(first, second):
        return first * jnp.where(is_state, jnp.exp(second[:, key : key + 1]), 1.0) + second

    diff = attend(
        [message for half in own for message in half], shared, mix_lambda, lam_other,
        head_gain[None, :], heads, halves, spans_low, sp,
    )
    step = 1
    while step < sp:
        heard = lax.ppermute(local, "sp", [(i, i ^ step) for i in range(sp)])
        if step == 1:
            heard = after(heard, packs[-1])
        if 2 * step >= sp:
            heard = after(heard, diff)
        upper = (s // step) % 2 == 1
        before = jnp.where(upper, join(heard, before), before)
        local = jnp.where(upper, join(heard, local), join(local, heard))
        step *= 2
    ret_out = retain(slabs, retain_log, parts, before, init_state, ret_heads, key, val, spans_low)

    home = [send(diff[r], unspread(r)) for r in range(heads)]
    low = lax.rem(z, heads)
    by_head = []
    for h in range(heads):
        block = home[0]
        for r in range(1, heads):
            block = jnp.where(lax.rem(low + r, heads) == h, home[r], block)
        by_head.append(block)
    mine = half_rows // CORES
    across = lambda p: lambda z, y, x, c: (z, y, (x + p) % halves, c)
    rows_of = lambda a, core: lax.dynamic_slice_in_dim(a, core * mine, mine, 0)

    def product(a, w):
        return jnp.dot(a, w, preferred_element_type=F32)

    outs = [
        jnp.concatenate([b[p] for b in by_head] + [ret_out[p]], axis=1) for p in range(halves)
    ]
    moved = [send(outs[p], across(p)) if p else outs[p] for p in range(halves)]
    pairs = []
    for q, w in enumerate(w_out):
        pairs.append((w, send(after(w, outs[-1] if q else own[-1]), other_core)))
    result = None
    for p in range(halves):
        theirs = send(rows_of(moved[p], 1 - c), other_core)
        for core, rows in enumerate((rows_of(moved[p], c), theirs)):
            term = product(rows, pairs[(halves - p) % halves][core])
            result = term if result is None else result + term
    return result.astype(BF16)


def solution(mesh):
    sp, tp = mesh.shape["sp"], mesh.shape["tp"]
    in_specs = (
        P(("sp", "tp"), None), P(),
        P(None, "tp"), P(None, "tp"), P(None, "tp"), P(None, "tp"), P(None, "tp"),
        P("tp"), P(),
        P(None, "tp"), P(None, "tp"), P(None, "tp"),
        P("tp", "sp"), P("tp", None, None), P("tp", None), P("tp", None),
    )

    def body(*args):
        return on_device(sp, tp, *args)

    return jax.shard_map(
        body, mesh=mesh, in_specs=in_specs, out_specs=P(("sp", "tp"), None), check_vma=False
    )
```
